32 devices in a mesh: sp: 2 (over x), dp: 16 (over z, y, core).
Axes of the slice: x: 2, y: 2, z: 4, core: 2. Of those that a mesh axis runs over, the one named last changes fastest.
Arguments:
- queries: bfloat16 [16, 384, 16, 128], P('dp', 'sp'), may hold values from -6 to 6
- keys: bfloat16 [16, 384, 16, 128], P('dp', 'sp'), may hold values from -6 to 6
- values: bfloat16 [16, 384, 16, 128], P('dp', 'sp'), may hold values from -6 to 6
- mix_ratio: float32 [16], replicated, may hold values from 0.3 to 0.8
- out_gain: float32 [128], replicated, may hold values from 0.1 to 1.9
- out_weight: bfloat16 [2048, 2048], P(None, 'dp'), may hold values from -0.125 to 0.125
Outputs:
- layer_out: bfloat16 [16, 384, 2048], P('dp', 'sp')
The draws below stay inside these ranges and needn't reach their ends.
All inputs are finite; a program needn't handle non-finite values.
Results may differ from the reference program's by a relative error of at most 0.0098.
Values may be sent and summed in bfloat16 or wider, within the bound.
A program may use at most 64 MiB of HBM per device.

```python
import math
import jax
import jax.numpy as jnp
from jax import lax

D = 2048
HEADS = 16
KEY_DIM = 64
HEAD_DIM = 128
SEQS = 16
LENGTH = 384


def score_field(key, salt):
    shape = (SEQS, LENGTH, HEADS, 2 * KEY_DIM)
    spread = jnp.clip(1.3 * jax.random.normal(jax.random.fold_in(key, salt), shape, jnp.float32), -6.0, 6.0)
    return spread.astype(jnp.bfloat16)


def draw_queries(key, part):
    return score_field(key, 1)


def draw_keys(key, part):
    return score_field(key, 2)


def block_levels(stream_key, dims, shards, smallest, high):
    level, own = 1.0, jax.random.fold_in(stream_key, 6)
    for dim, blocks in shards:
        heights = jnp.exp(jax.random.uniform(jax.random.fold_in(own, dim), (blocks,), jnp.float32, smallest / len(shards), high / len(shards)))
        level = level * jnp.repeat(heights, dims[dim] // blocks).reshape([-1 if axis == dim else 1 for axis in range(len(dims))])
    return level


def bell_draw(rng, shape, scale, bound, pieces=(), kind=jnp.bfloat16):
    loudness = block_levels(rng, shape, pieces, -0.22, 0.18) if pieces else 1.0
    array = jax.random.normal(rng, shape, jnp.float32) * scale * loudness
    return jnp.minimum(jnp.maximum(array, -bound), bound).astype(kind)


def setup_inputs(seed: int = 0) -> dict:
    streams_of = jax.random.split(jax.random.key(seed), 7)
    return {
        "queries": draw_queries(jax.random.fold_in(streams_of[6], 71), 0),
        "keys": draw_keys(jax.random.fold_in(streams_of[6], 71), 0),
        "values": bell_draw(streams_of[2], (SEQS, LENGTH, HEADS, HEAD_DIM), 1.0, 6.0, ((0, 16), (1, 2))),
        "mix_ratio": jnp.clip(jax.random.uniform(streams_of[3], (HEADS,), jnp.float32, 0.3, 0.8), 0.3, 0.8),
        "out_gain": jnp.clip(1.0 + 0.18 * jax.random.normal(streams_of[4], (HEAD_DIM,), jnp.float32), 0.1, 1.9),
        "out_weight": bell_draw(streams_of[5], (HEADS * HEAD_DIM, D), (HEADS * HEAD_DIM) ** -0.5, 0.125, ((1, 16),)),
    }


theta_base = 500000.0
neg_large = -1e+30
norm_eps = 1e-05

def rotate_halves(field, positions):
    width = field.shape[-1] // 2
    half = width // 2
    freqs = theta_base ** (-jnp.arange(half, dtype=jnp.float32) * 2.0 / width)
    angle = positions.astype(jnp.float32)[:, None] * freqs[None, :]
    cosine = jnp.cos(angle)[:, None, :]
    sine = jnp.sin(angle)[:, None, :]
    parts = field.reshape(field.shape[0], 2, width)
    lower = parts[..., :half]
    upper = parts[..., half:]
    turned = jnp.concatenate([lower * cosine - upper * sine, upper * cosine + lower * sine], axis=-1)
    return turned.reshape(field.shape)

def masked_softmax(scores, visible):
    kept = jnp.where(visible, scores, neg_large)
    highest = lax.optimization_barrier(jnp.max(kept, axis=-1, keepdims=True))
    powers = jnp.exp(kept - highest)
    return powers / lax.optimization_barrier(jnp.sum(powers, axis=-1, keepdims=True))

def head_attention(query_head, key_head, value_head, ratio, gain):
    length = query_head.shape[0]
    width = query_head.shape[1] // 2
    positions = jnp.arange(length, dtype=jnp.int32)
    rotated_queries = (rotate_halves(query_head.astype(jnp.float32), positions) * width ** (-0.5)).astype(jnp.bfloat16)
    rotated_keys = rotate_halves(key_head.astype(jnp.float32), positions).astype(jnp.bfloat16)
    block = math.gcd(512, length)

    def one_block(start):
        query_rows = lax.dynamic_slice_in_dim(rotated_queries, start, block, 0)
        visible = (start + jnp.arange(block, dtype=jnp.int32))[:, None] >= positions[None, :]
        first = jnp.dot(query_rows[:, :width], rotated_keys[:, :width].T, preferred_element_type=jnp.float32)
        second = jnp.dot(query_rows[:, width:], rotated_keys[:, width:].T, preferred_element_type=jnp.float32)
        weights = (masked_softmax(first, visible) - ratio * masked_softmax(second, visible)).astype(jnp.bfloat16)
        mixed = jnp.dot(weights, value_head, preferred_element_type=jnp.float32)
        scale = lax.rsqrt(lax.optimization_barrier(jnp.mean(mixed * mixed, axis=-1, keepdims=True)) + norm_eps)
        return (mixed * scale * gain).astype(jnp.bfloat16)
    starts = jnp.arange(length // block, dtype=jnp.int32) * block
    return lax.map(one_block, starts).reshape(length, value_head.shape[1])

def reference(queries, keys, values, mix_ratio, out_gain, out_weight):

    def one_sequence(items):
        query_seq, key_seq, value_seq = items

        def one_head(head_items):
            query_head, key_head, value_head, ratio = head_items
            return head_attention(query_head, key_head, value_head, ratio, out_gain)
        heads = lax.map(one_head, (jnp.swapaxes(query_seq, 0, 1), jnp.swapaxes(key_seq, 0, 1), jnp.swapaxes(value_seq, 0, 1), mix_ratio))
        attended = jnp.swapaxes(heads, 0, 1).reshape(query_seq.shape[0], -1)
        return jnp.dot(attended, out_weight, preferred_element_type=jnp.float32).astype(jnp.bfloat16)
    return lax.map(one_sequence, (queries, keys, values))
```

```python
import functools
import math

import jax
import jax.numpy as jnp
import numpy as np
from jax import lax
from jax.experimental import pallas as pl
from jax.experimental.pallas import tpu as pltpu
from jax.sharding import PartitionSpec as P

theta_base = 500000.0
neg_large = -1e30
norm_eps = 1e-05
MESH = pl.DeviceIdType.MESH


def rotate_halves(field, positions):
    width = field.shape[-1] // 2
    half = width // 2
    freqs = theta_base ** (-jnp.arange(half, dtype=jnp.float32) * 2.0 / width)
    angle = positions.astype(jnp.float32)[:, None] * freqs[None, :]
    cosine = jnp.cos(angle)[:, None, :]
    sine = jnp.sin(angle)[:, None, :]
    parts = field.reshape(field.shape[0], 2, width)
    lower = parts[..., :half]
    upper = parts[..., half:]
    turned = jnp.concatenate(
        [lower * cosine - upper * sine, upper * cosine + lower * sine], axis=-1
    )
    return turned.reshape(field.shape)


def masked_softmax(scores, visible):
    kept = jnp.where(visible, scores, neg_large)
    highest = jnp.max(kept, axis=-1, keepdims=True)
    powers = jnp.exp(kept - highest)
    return powers / jnp.sum(powers, axis=-1, keepdims=True)


def head_attention(query_head, key_head, value_head, ratio, gain):
    length = query_head.shape[0]
    width = query_head.shape[1] // 2
    positions = jnp.arange(length, dtype=jnp.int32)
    rotated_queries = (
        rotate_halves(query_head.astype(jnp.float32), positions) * width ** (-0.5)
    ).astype(jnp.bfloat16)
    rotated_keys = rotate_halves(key_head.astype(jnp.float32), positions).astype(jnp.bfloat16)
    block = math.gcd(512, length)

    def one_block(start):
        query_rows = lax.dynamic_slice_in_dim(rotated_queries, start, block, 0)
        visible = (start + jnp.arange(block, dtype=jnp.int32))[:, None] >= positions[None, :]
        first = jnp.dot(
            query_rows[:, :width], rotated_keys[:, :width].T, preferred_element_type=jnp.float32
        )
        second = jnp.dot(
            query_rows[:, width:], rotated_keys[:, width:].T, preferred_element_type=jnp.float32
        )
        weights = (masked_softmax(first, visible) - ratio * masked_softmax(second, visible)).astype(
            jnp.bfloat16
        )
        mixed = jnp.dot(weights, value_head, preferred_element_type=jnp.float32)
        scale = lax.rsqrt(jnp.mean(mixed * mixed, axis=-1, keepdims=True) + norm_eps)
        return (mixed * scale * gain).astype(jnp.bfloat16)

    starts = jnp.arange(length // block, dtype=jnp.int32) * block
    return lax.map(one_block, starts).reshape(length, value_head.shape[1])


def on_device(queries, keys, values, mix_ratio, out_gain, out_weight):
    groups = lax.axis_size("sp")
    heads_here = queries.shape[2] // groups
    query_all, key_all, value_all = (
        lax.all_to_all(queries, "sp", split_axis=2, concat_axis=1, tiled=True),
        lax.all_to_all(keys, "sp", split_axis=2, concat_axis=1, tiled=True),
        lax.all_to_all(values, "sp", split_axis=2, concat_axis=1, tiled=True),
    )
    seqs = query_all.shape[0]
    length = query_all.shape[1]
    first_head = lax.axis_index("sp") * heads_here
    ratios = lax.dynamic_slice_in_dim(mix_ratio, first_head, heads_here, 0)
    item_ratios = jnp.tile(ratios, seqs)

    def by_item(field):
        return jnp.swapaxes(field, 1, 2).reshape(seqs * heads_here, length, field.shape[3])

    def one_head(head_items):
        query_head, key_head, value_head, ratio = head_items
        return head_attention(query_head, key_head, value_head, ratio, out_gain)

    heads = lax.map(
        one_head, (by_item(query_all), by_item(key_all), by_item(value_all), item_ratios)
    )
    attended = jnp.swapaxes(heads.reshape(seqs, heads_here, length, heads.shape[2]), 1, 2)
    returned = lax.all_to_all(attended, "sp", split_axis=1, concat_axis=2, tiled=True)
    tokens_here = returned.shape[1]
    token_rows = returned.reshape(seqs * tokens_here, -1)
    result = jnp.dot(
        token_rows,
        lax.all_gather(out_weight, "dp", axis=1, tiled=True),
        preferred_element_type=jnp.float32,
    ).astype(jnp.bfloat16)
    return result.reshape(seqs, tokens_here, -1)


def rotation_tables(length, width):
    half = width // 2
    freqs = theta_base ** (-np.arange(half, dtype=np.float32) * np.float32(2.0) / width)
    angle = np.arange(length, dtype=np.float32)[:, None] * freqs.astype(np.float32)[None, :]
    cosine, sine = np.cos(angle), np.sin(angle)
    return (
        np.tile(cosine, (1, 4)).astype(np.float32),
        np.tile(sine, (1, 4)).astype(np.float32),
    )


def turning_matrix(width):
    half = width // 2
    turn = np.zeros((2 * width, 2 * width), np.float32)
    for part in range(2):
        for j in range(half):
            turn[part * width + half + j, part * width + j] = -1.0
            turn[part * width + j, part * width + half + j] = 1.0
    return turn


def pick(table, index):
    value = jnp.int32(table[0])
    for i, entry in enumerate(table[1:], 1):
        value = jnp.where(index == i, jnp.int32(entry), value)
    return value


def line_kernel(
    depth_z, heads, pieces, mix_ref, q_ref, k_ref, v_ref, cos_ref, sin_ref, turn_ref, gain_ref, w_ref,
    out_ref, far_k, far_v, wall, attended,
    k_send, v_send, k_recv, v_recv, w_recv, up_send, down_send, side_send, core_send, extra_send, own_sem,
):
    s = lax.axis_index("sp")
    d = lax.axis_index("dp")
    c = lax.rem(d, 2)
    y = lax.rem(d // 2, 2)
    z = d // 4
    tokens = q_ref.shape[0]
    size = q_ref.shape[1] // heads
    width = size // 2
    columns = w_ref.shape[1]
    rows = w_ref.shape[0] // pieces

    def at(zz, yy, cc):
        return {"sp": s, "dp": (zz * 2 + yy) * 2 + cc}

    across = {"sp": 1 - s, "dp": d}
    barrier = pltpu.get_barrier_semaphore()

    def greet(target):
        pl.semaphore_signal(barrier, inc=1, device_id=target, device_id_type=MESH)

    greet(across)
    greet(at(z, 1 - y, c))
    greet(at(z, y, 1 - c))

    @pl.when(z > 0)
    def _():
        greet(at(z - 1, y, c))

    @pl.when(z < depth_z - 1)
    def _():
        greet(at(z + 1, y, c))

    pl.semaphore_wait(
        barrier,
        3 + jnp.where(z > 0, 1, 0).astype(jnp.int32) + jnp.where(z < depth_z - 1, 1, 0).astype(jnp.int32),
    )

    def place(zz, yy, cc, q):
        column = pl.multiple_of(((zz * 2 + yy) * 2 + cc) * columns, columns)
        return wall.at[pl.ds(q * rows, rows), pl.ds(column, columns)]

    def send(zz, yy, cc, q, sem, target, own):
        where = place(zz, yy, cc, q)
        return pltpu.make_async_remote_copy(
            src_ref=w_ref.at[pl.ds(q * rows, rows), :] if own else where,
            dst_ref=where,
            send_sem=sem,
            recv_sem=w_recv.at[zz, yy, cc, q],
            device_id=target,
            device_id_type=MESH,
        )

    near = z + 1 - 2 * lax.rem(z, 2)

    def to_up(zz, q, own=False):
        return send(zz, y, c, q, up_send.at[zz, q], at(z + 1, y, c), own)

    def to_down(zz, q, own=False):
        return send(zz, y, c, q, down_send.at[zz, q], at(z - 1, y, c), own)

    def to_side(zz, q, own=False):
        return send(zz, y, c, q, side_send.at[zz, q], at(z, 1 - y, c), own)

    def to_core(zz, yy, q, own=False):
        return send(zz, yy, c, q, core_send.at[zz, yy, q], at(z, y, 1 - c), own)

    def to_near(q):
        return send(z, 1 - y, c, q, extra_send.at[q], at(near, y, c), False)

    def arrived(zz, yy, cc, q):
        send(zz, yy, cc, q, side_send.at[0, 0], at(z, 1 - y, c), False).wait_recv()

    def head_at(h):
        return pl.ds(pl.multiple_of(h * size, size), size)

    def far_copy(h, src, dst, sends, recvs):
        return pltpu.make_async_remote_copy(
            src_ref=src.at[:, head_at(h)],
            dst_ref=dst.at[:, head_at(h)],
            send_sem=sends.at[h],
            recv_sem=recvs.at[h],
            device_id=across,
            device_id_type=MESH,
        )

    for q in range(pieces):

        @pl.when(z > 0)
        def _(q=q):
            to_down(z, q, True).start()

        @pl.when(z < depth_z - 1)
        def _(q=q):
            to_up(z, q, True).start()

        to_side(z, q, True).start()
        to_core(z, y, q, True).start()

    @pl.when(s == 0)
    def _():
        def start(h, carry):
            far_copy(h, k_ref, far_k, k_send, k_recv).start()
            far_copy(h, v_ref, far_v, v_send, v_recv).start()
            return carry

        lax.fori_loop(0, heads, start, 0)

    own_copy = pltpu.make_async_copy(
        w_ref, wall.at[:, pl.ds(pl.multiple_of(d * columns, columns), columns)], own_sem
    )
    own_copy.start()

    late = pieces // 2

    def line_arrival(r, q):
        for sign in (-1, 1):
            zz = z + sign * r

            @pl.when((zz >= 0) & (zz < depth_z))
            def _(zz=zz, sign=sign):
                arrived(zz, y, c, q)
                if sign < 0:

                    @pl.when(z < depth_z - 1)
                    def _():
                        to_up(zz, q).start()
                else:

                    @pl.when(z > 0)
                    def _():
                        to_down(zz, q).start()

                if q < late:
                    to_side(zz, q).start()
                else:

                    @pl.when(zz != near)
                    def _():
                        to_side(zz, q).start()

                to_core(zz, y, q).start()

    def side_arrival(r, q):
        if r == 0:
            arrived(z, 1 - y, c, q)
            to_core(z, 1 - y, q).start()
            return
        for sign in (-1, 1):
            zz = z + sign * r
            here = (zz >= 0) & (zz < depth_z)
            if q >= late:
                here = here & (zz != near)

            @pl.when(here)
            def _(zz=zz):
                arrived(zz, 1 - y, c, q)
                to_core(zz, 1 - y, q).start()

    def extra(q):
        to_near(q).start()

    def extra_arrival(q):
        arrived(near, 1 - y, c, q)
        to_core(near, 1 - y, q).start()

    block_time = 4.0 * heads / 12.0
    events = []
    for q in range(pieces):
        step = (q + 1) / pieces
        for r in range(1, depth_z):
            events.append((block_time * (r - 1 + step), functools.partial(line_arrival, r, q)))
            events.append((block_time * (r + step) + 1.0, functools.partial(side_arrival, r, q)))
        events.append((block_time * step + 1.0, functools.partial(side_arrival, 0, q)))
        if q >= late:
            events.append((block_time * (depth_z - 2) + 0.5 + 0.01 * q, functools.partial(extra, q)))
            events.append((block_time * (depth_z - 1 + step) + 1.5, functools.partial(extra_arrival, q)))
    events.sort(key=lambda e: e[0])

    lane = lax.broadcasted_iota(jnp.int32, (tokens, size), 1)
    visible = lax.broadcasted_iota(jnp.int32, (tokens, tokens), 0) >= lax.broadcasted_iota(
        jnp.int32, (tokens, tokens), 1
    )
    my_rows = pl.ds(pl.multiple_of(s * tokens, 8), tokens)

    def turned(field, table_rows):
        crossed = jnp.dot(field, turn_ref[...], preferred_element_type=jnp.float32)
        return field.astype(jnp.float32) * cos_ref[table_rows, :] + crossed * sin_ref[table_rows, :]

    def product(a, b):
        return lax.dot_general(a, b, (((1,), (1,)), ((), ())), preferred_element_type=jnp.float32)

    def queries_of(h):
        query = (turned(q_ref[:, head_at(h)], my_rows) * width ** (-0.5)).astype(jnp.bfloat16)
        zero = jnp.zeros_like(query)
        return jnp.where(lane < width, query, zero), jnp.where(lane < width, zero, query)

    def finish(h, mixed):
        scale = lax.rsqrt(jnp.mean(mixed * mixed, axis=-1, keepdims=True) + norm_eps)
        attended[:, head_at(h)] = (mixed * scale * gain_ref[...]).astype(jnp.bfloat16)

    def near_only(h):
        key = turned(k_ref[:, head_at(h)], my_rows).astype(jnp.bfloat16)
        maps = []
        for query in queries_of(h):
            scores = jnp.where(visible, product(query, key), neg_large)
            powers = jnp.exp(scores - jnp.max(scores, axis=-1, keepdims=True))
            maps.append((powers, jnp.sum(powers, axis=-1, keepdims=True)))
        (first, first_sum), (second, second_sum) = maps
        weights = first * (1.0 / first_sum) - second * (mix_ref[h] / second_sum)
        finish(
            h,
            jnp.dot(weights.astype(jnp.bfloat16), v_ref[:, head_at(h)], preferred_element_type=jnp.float32),
        )

    def near_and_far(h):
        key = turned(k_ref[:, head_at(h)], my_rows).astype(jnp.bfloat16)
        far_key = turned(far_k[:, head_at(h)], pl.ds(0, tokens)).astype(jnp.bfloat16)
        maps = []
        for query in queries_of(h):
            scores = jnp.where(visible, product(query, key), neg_large)
            far_scores = product(query, far_key)
            highest = jnp.maximum(
                jnp.max(scores, axis=-1, keepdims=True), jnp.max(far_scores, axis=-1, keepdims=True)
            )
            powers = jnp.exp(scores - highest)
            far_powers = jnp.exp(far_scores - highest)
            total = jnp.sum(powers, axis=-1, keepdims=True) + jnp.sum(far_powers, axis=-1, keepdims=True)
            maps.append((powers, far_powers, total))
        (first, far_first, first_sum), (second, far_second, second_sum) = maps
        one, two = 1.0 / first_sum, mix_ref[h] / second_sum
        weights = (first * one - second * two).astype(jnp.bfloat16)
        far_weights = (far_first * one - far_second * two).astype(jnp.bfloat16)
        finish(
            h,
            jnp.dot(weights, v_ref[:, head_at(h)], preferred_element_type=jnp.float32)
            + jnp.dot(far_weights, far_v[:, head_at(h)], preferred_element_type=jnp.float32),
        )

    def head_step(h, carry):
        for when, action in events:
            turn = max(0, int(when))
            if turn < heads:
                pl.when(h == turn)(action)

        @pl.when(s == 0)
        def _():
            near_only(h)

        @pl.when(s == 1)
        def _():
            far_copy(h, k_ref, far_k, k_send, k_recv).wait_recv()
            far_copy(h, v_ref, far_v, v_send, v_recv).wait_recv()
            near_and_far(h)

        return carry

    lax.fori_loop(0, heads, head_step, 0)
    own_copy.wait()
    for when, action in events:
        if max(0, int(when)) >= heads:
            action()

    orders = [sorted(range(depth_z), key=lambda b: (abs(b - a), b)) for a in range(depth_z)]
    for n in range(depth_z):
        zz = pick([order[n] for order in orders], z)
        for yy in (y, 1 - y):

            for q in range(pieces):
                arrived(zz, yy, 1 - c, q)
            chip = pl.ds(pl.multiple_of((zz * 2 + yy) * 2 * columns, 2 * columns), 2 * columns)
            out_ref[:, chip] = jnp.dot(
                attended[...], wall[:, chip], preferred_element_type=jnp.float32
            ).astype(out_ref.dtype)

    for q in range(pieces):
        for b in range(depth_z):
            passed_up = (b <= z) & (z < depth_z - 1)
            passed_down = (b >= z) & (z > 0)

            @pl.when(passed_up)
            def _(b=b):
                to_up(b, q).wait_send()

            @pl.when(passed_down)
            def _(b=b):
                to_down(b, q).wait_send()

            if q < late:
                to_side(b, q).wait_send()
            else:

                @pl.when(b != near)
                def _(b=b):
                    to_side(b, q).wait_send()

            for yy in range(2):
                to_core(b, yy, q).wait_send()
        if q >= late:
            to_near(q).wait_send()

    @pl.when(s == 0)
    def _():
        def ended(h, carry):
            far_copy(h, k_ref, far_k, k_send, k_recv).wait_send()
            far_copy(h, v_ref, far_v, v_send, v_recv).wait_send()
            return carry

        lax.fori_loop(0, heads, ended, 0)


def lines_of(mesh):
    names = tuple(mesh.axis_names)
    if names != ("sp", "dp") or mesh.shape["sp"] != 2 or mesh.shape["dp"] % 4:
        return None
    depth_z = mesh.shape["dp"] // 4
    return depth_z if depth_z >= 4 and depth_z % 2 == 0 else None


def on_line(depth_z, queries, keys, values, mix_ratio, out_gain, out_weight):
    _, tokens, heads, size = queries.shape
    features = heads * size
    pieces = 4
    cosine, sine = rotation_tables(2 * tokens, size // 2)
    flat = [field.reshape(tokens, features) for field in (queries, keys, values)]
    vmem = pl.BlockSpec(memory_space=pltpu.VMEM)
    smem = pl.BlockSpec(memory_space=pltpu.SMEM)
    dma = pltpu.SemaphoreType.DMA
    result = pl.pallas_call(
        functools.partial(line_kernel, depth_z, heads, pieces),
        out_shape=jax.ShapeDtypeStruct((tokens, features), jnp.bfloat16),
        in_specs=[smem] + [vmem] * 8,
        out_specs=vmem,
        scratch_shapes=[
            pltpu.VMEM((tokens, features), jnp.bfloat16),
            pltpu.VMEM((tokens, features), jnp.bfloat16),
            pltpu.VMEM((features, out_weight.shape[1] * depth_z * 4), jnp.bfloat16),
            pltpu.VMEM((tokens, features), jnp.bfloat16),
            dma((heads,)),
            dma((heads,)),
            dma((heads,)),
            dma((heads,)),
            dma((depth_z, 2, 2, pieces)),
            dma((depth_z, pieces)),
            dma((depth_z, pieces)),
            dma((depth_z, pieces)),
            dma((depth_z, 2, pieces)),
            dma((pieces,)),
            dma,
        ],
        compiler_params=pltpu.CompilerParams(
            collective_id=0, has_side_effects=True, vmem_limit_bytes=56 * 2**20
        ),
    )(
        mix_ratio,
        *flat,
        jnp.asarray(cosine),
        jnp.asarray(sine),
        jnp.asarray(turning_matrix(size // 2), jnp.bfloat16),
        out_gain.reshape(1, size),
        out_weight,
    )
    return result.reshape(1, tokens, features)


def solution(mesh):
    in_specs = (
        P("dp", "sp", None, None),
        P("dp", "sp", None, None),
        P("dp", "sp", None, None),
        P(),
        P(),
        P(None, "dp"),
    )
    out_specs = P("dp", "sp", None)
    depth_z = lines_of(mesh)

    def body(queries, *rest):
        fits = depth_z is not None and queries.shape[0] == 1 and queries.shape[1] <= 256
        return functools.partial(on_line, depth_z)(queries, *rest) if fits else on_device(queries, *rest)

    return jax.shard_map(body, mesh=mesh, in_specs=in_specs, out_specs=out_specs, check_vma=False)
```

```python
import functools
import math

import jax
import jax.numpy as jnp
import numpy as np
from jax import lax
from jax.experimental import pallas as pl
from jax.experimental.pallas import tpu as pltpu
from jax.sharding import PartitionSpec as P

theta_base = 500000.0
neg_large = -1e30
norm_eps = 1e-05
MESH = pl.DeviceIdType.MESH


def rotate_halves(field, positions):
    width = field.shape[-1] // 2
    half = width // 2
    freqs = theta_base ** (-jnp.arange(half, dtype=jnp.float32) * 2.0 / width)
    angle = positions.astype(jnp.float32)[:, None] * freqs[None, :]
    cosine = jnp.cos(angle)[:, None, :]
    sine = jnp.sin(angle)[:, None, :]
    parts = field.reshape(field.shape[0], 2, width)
    lower = parts[..., :half]
    upper = parts[..., half:]
    turned = jnp.concatenate(
        [lower * cosine - upper * sine, upper * cosine + lower * sine], axis=-1
    )
    return turned.reshape(field.shape)


def masked_softmax(scores, visible):
    kept = jnp.where(visible, scores, neg_large)
    highest = jnp.max(kept, axis=-1, keepdims=True)
    powers = jnp.exp(kept - highest)
    return powers / jnp.sum(powers, axis=-1, keepdims=True)


def head_attention(query_head, key_head, value_head, ratio, gain):
    length = query_head.shape[0]
    width = query_head.shape[1] // 2
    positions = jnp.arange(length, dtype=jnp.int32)
    rotated_queries = (
        rotate_halves(query_head.astype(jnp.float32), positions) * width ** (-0.5)
    ).astype(jnp.bfloat16)
    rotated_keys = rotate_halves(key_head.astype(jnp.float32), positions).astype(jnp.bfloat16)
    block = math.gcd(512, length)

    def one_block(start):
        query_rows = lax.dynamic_slice_in_dim(rotated_queries, start, block, 0)
        visible = (start + jnp.arange(block, dtype=jnp.int32))[:, None] >= positions[None, :]
        first = jnp.dot(
            query_rows[:, :width], rotated_keys[:, :width].T, preferred_element_type=jnp.float32
        )
        second = jnp.dot(
            query_rows[:, width:], rotated_keys[:, width:].T, preferred_element_type=jnp.float32
        )
        weights = (masked_softmax(first, visible) - ratio * masked_softmax(second, visible)).astype(
            jnp.bfloat16
        )
        mixed = jnp.dot(weights, value_head, preferred_element_type=jnp.float32)
        scale = lax.rsqrt(jnp.mean(mixed * mixed, axis=-1, keepdims=True) + norm_eps)
        return (mixed * scale * gain).astype(jnp.bfloat16)

    starts = jnp.arange(length // block, dtype=jnp.int32) * block
    return lax.map(one_block, starts).reshape(length, value_head.shape[1])


def on_device(queries, keys, values, mix_ratio, out_gain, out_weight):
    groups = lax.axis_size("sp")
    heads_here = queries.shape[2] // groups
    query_all, key_all, value_all = (
        lax.all_to_all(queries, "sp", split_axis=2, concat_axis=1, tiled=True),
        lax.all_to_all(keys, "sp", split_axis=2, concat_axis=1, tiled=True),
        lax.all_to_all(values, "sp", split_axis=2, concat_axis=1, tiled=True),
    )
    seqs = query_all.shape[0]
    length = query_all.shape[1]
    first_head = lax.axis_index("sp") * heads_here
    ratios = lax.dynamic_slice_in_dim(mix_ratio, first_head, heads_here, 0)
    item_ratios = jnp.tile(ratios, seqs)

    def by_item(field):
        return jnp.swapaxes(field, 1, 2).reshape(seqs * heads_here, length, field.shape[3])

    def one_head(head_items):
        query_head, key_head, value_head, ratio = head_items
        return head_attention(query_head, key_head, value_head, ratio, out_gain)

    heads = lax.map(
        one_head, (by_item(query_all), by_item(key_all), by_item(value_all), item_ratios)
    )
    attended = jnp.swapaxes(heads.reshape(seqs, heads_here, length, heads.shape[2]), 1, 2)
    returned = lax.all_to_all(attended, "sp", split_axis=1, concat_axis=2, tiled=True)
    tokens_here = returned.shape[1]
    token_rows = returned.reshape(seqs * tokens_here, -1)
    result = jnp.dot(
        token_rows,
        lax.all_gather(out_weight, "dp", axis=1, tiled=True),
        preferred_element_type=jnp.float32,
    ).astype(jnp.bfloat16)
    return result.reshape(seqs, tokens_here, -1)


def rotation_tables(length, width):
    half = width // 2
    freqs = theta_base ** (-np.arange(half, dtype=np.float32) * np.float32(2.0) / width)
    angle = np.arange(length, dtype=np.float32)[:, None] * freqs.astype(np.float32)[None, :]
    cosine, sine = np.cos(angle), np.sin(angle)
    return (
        np.tile(cosine, (1, 4)).astype(np.float32),
        np.tile(sine, (1, 4)).astype(np.float32),
    )


def turning_matrix(width):
    half = width // 2
    turn = np.zeros((2 * width, 2 * width), np.float32)
    for part in range(2):
        for j in range(half):
            turn[part * width + half + j, part * width + j] = -1.0
            turn[part * width + j, part * width + half + j] = 1.0
    return turn


def pick(table, index):
    value = jnp.int32(table[0])
    for i, entry in enumerate(table[1:], 1):
        value = jnp.where(index == i, jnp.int32(entry), value)
    return value


def line_kernel(
    depth_z, heads, pieces, mix_ref, q_in, k_in, v_in, cos_in, sin_in, turn_ref, gain_ref, w_in,
    out_ref, q_raw, k_raw, v_raw, cos_ref, sin_ref, w_ref, q_ref, k_ref, v_ref, far_k, far_v, wall, attended, in_sems,
    k_send, v_send, k_recv, v_recv, w_recv, up_send, down_send, side_send, core_send, extra_send, own_sem,
):
    s = lax.axis_index("sp")
    d = lax.axis_index("dp")
    c = lax.rem(d, 2)
    y = lax.rem(d // 2, 2)
    z = d // 4
    tokens = q_ref.shape[0]
    size = q_ref.shape[1] // heads
    width = size // 2
    columns = w_ref.shape[1]
    rows = w_ref.shape[0] // pieces

    def at(zz, yy, cc):
        return {"sp": s, "dp": (zz * 2 + yy) * 2 + cc}

    across = {"sp": 1 - s, "dp": d}
    loads = [
        pltpu.make_async_copy(src, dst, in_sems.at[i])
        for i, (src, dst) in enumerate(
            [(w_in, w_ref), (k_in, k_raw), (v_in, v_raw), (q_in, q_raw), (cos_in, cos_ref), (sin_in, sin_ref)]
        )
    ]
    for load in loads:
        load.start()
    barrier = pltpu.get_barrier_semaphore()

    def greet(target):
        pl.semaphore_signal(barrier, inc=1, device_id=target, device_id_type=MESH)

    greet(across)
    greet(at(z, 1 - y, c))
    greet(at(z, y, 1 - c))

    @pl.when(z > 0)
    def _():
        greet(at(z - 1, y, c))

    @pl.when(z < depth_z - 1)
    def _():
        greet(at(z + 1, y, c))

    pl.semaphore_wait(
        barrier,
        3 + jnp.where(z > 0, 1, 0).astype(jnp.int32) + jnp.where(z < depth_z - 1, 1, 0).astype(jnp.int32),
    )

    loads[0].wait()

    def place(zz, yy, cc, q):
        column = pl.multiple_of(((zz * 2 + yy) * 2 + cc) * columns, columns)
        return wall.at[pl.ds(q * rows, rows), pl.ds(column, columns)]

    def send(zz, yy, cc, q, sem, target, own):
        where = place(zz, yy, cc, q)
        return pltpu.make_async_remote_copy(
            src_ref=w_ref.at[pl.ds(q * rows, rows), :] if own else where,
            dst_ref=where,
            send_sem=sem,
            recv_sem=w_recv.at[zz, yy, cc, q],
            device_id=target,
            device_id_type=MESH,
        )

    near = z + 1 - 2 * lax.rem(z, 2)

    def to_up(zz, q, own=False):
        return send(zz, y, c, q, up_send.at[zz, q], at(z + 1, y, c), own)

    def to_down(zz, q, own=False):
        return send(zz, y, c, q, down_send.at[zz, q], at(z - 1, y, c), own)

    def to_side(zz, q, own=False):
        return send(zz, y, c, q, side_send.at[zz, q], at(z, 1 - y, c), own)

    def to_core(zz, yy, q, own=False):
        return send(zz, yy, c, q, core_send.at[zz, yy, q], at(z, y, 1 - c), own)

    def to_near(q):
        return send(z, 1 - y, c, q, extra_send.at[q], at(near, y, c), False)

    def arrived(zz, yy, cc, q):
        send(zz, yy, cc, q, side_send.at[0, 0], at(z, 1 - y, c), False).wait_recv()

    def head_at(h):
        return pl.ds(pl.multiple_of(h * size, size), size)

    def far_copy(h, src, dst, sends, recvs):
        return pltpu.make_async_remote_copy(
            src_ref=src.at[:, head_at(h)],
            dst_ref=dst.at[:, head_at(h)],
            send_sem=sends.at[h],
            recv_sem=recvs.at[h],
            device_id=across,
            device_id_type=MESH,
        )

    for q in range(pieces):

        @pl.when(z > 0)
        def _(q=q):
            to_down(z, q, True).start()

        @pl.when(z < depth_z - 1)
        def _(q=q):
            to_up(z, q, True).start()

        to_side(z, q, True).start()
        to_core(z, y, q, True).start()

    def flatten(src, dst):
        rows_now = math.gcd(16, tokens)

        def some(i, carry):
            part = pl.ds(pl.multiple_of(i * rows_now, rows_now), rows_now)
            dst[part, :] = src[part, :, :].reshape(rows_now, heads * size)
            return carry

        lax.fori_loop(0, tokens // rows_now, some, 0)

    for load, src, dst in ((loads[1], k_raw, k_ref), (loads[2], v_raw, v_ref), (loads[3], q_raw, q_ref)):
        load.wait()
        flatten(src, dst)

    @pl.when(s == 0)
    def _():
        def start(h, carry):
            far_copy(h, k_ref, far_k, k_send, k_recv).start()
            far_copy(h, v_ref, far_v, v_send, v_recv).start()
            return carry

        lax.fori_loop(0, heads, start, 0)

    own_copy = pltpu.make_async_copy(
        w_ref, wall.at[:, pl.ds(pl.multiple_of(d * columns, columns), columns)], own_sem
    )
    own_copy.start()
    loads[4].wait()
    loads[5].wait()

    late = pieces // 2

    def line_arrival(r, q):
        for sign in (-1, 1):
            zz = z + sign * r

            @pl.when((zz >= 0) & (zz < depth_z))
            def _(zz=zz, sign=sign):
                arrived(zz, y, c, q)
                if sign < 0:

                    @pl.when(z < depth_z - 1)
                    def _():
                        to_up(zz, q).start()
                else:

                    @pl.when(z > 0)
                    def _():
                        to_down(zz, q).start()

                if q < late:
                    to_side(zz, q).start()
                else:

                    @pl.when(zz != near)
                    def _():
                        to_side(zz, q).start()

                to_core(zz, y, q).start()

    def side_arrival(r, q):
        if r == 0:
            arrived(z, 1 - y, c, q)
            to_core(z, 1 - y, q).start()
            return
        for sign in (-1, 1):
            zz = z + sign * r
            here = (zz >= 0) & (zz < depth_z)
            if q >= late:
                here = here & (zz != near)

            @pl.when(here)
            def _(zz=zz):
                arrived(zz, 1 - y, c, q)
                to_core(zz, 1 - y, q).start()

    def extra(q):
        to_near(q).start()

    def extra_arrival(q):
        arrived(near, 1 - y, c, q)
        to_core(near, 1 - y, q).start()

    block_time = 4.0 * heads / 12.0
    events = []
    for q in range(pieces):
        step = (q + 1) / pieces
        for r in range(1, depth_z):
            events.append((block_time * (r - 1 + step), functools.partial(line_arrival, r, q)))
            events.append((block_time * (r + step) + 1.0, functools.partial(side_arrival, r, q)))
        events.append((block_time * step + 1.0, functools.partial(side_arrival, 0, q)))
        if q >= late:
            events.append((block_time * (depth_z - 2) + 0.5 + 0.01 * q, functools.partial(extra, q)))
            events.append((block_time * (depth_z - 1 + step) + 1.5, functools.partial(extra_arrival, q)))
    events.sort(key=lambda e: e[0])

    lane = lax.broadcasted_iota(jnp.int32, (tokens, size), 1)
    visible = lax.broadcasted_iota(jnp.int32, (tokens, tokens), 0) >= lax.broadcasted_iota(
        jnp.int32, (tokens, tokens), 1
    )
    my_rows = pl.ds(pl.multiple_of(s * tokens, 8), tokens)

    def turned(field, table_rows):
        crossed = jnp.dot(field, turn_ref[...], preferred_element_type=jnp.float32)
        return field.astype(jnp.float32) * cos_ref[table_rows, :] + crossed * sin_ref[table_rows, :]

    def product(a, b):
        return lax.dot_general(a, b, (((1,), (1,)), ((), ())), preferred_element_type=jnp.float32)

    def queries_of(h):
        query = (turned(q_ref[:, head_at(h)], my_rows) * width ** (-0.5)).astype(jnp.bfloat16)
        zero = jnp.zeros_like(query)
        return jnp.where(lane < width, query, zero), jnp.where(lane < width, zero, query)

    def finish(h, mixed):
        scale = lax.rsqrt(jnp.mean(mixed * mixed, axis=-1, keepdims=True) + norm_eps)
        attended[:, head_at(h)] = (mixed * scale * gain_ref[...]).astype(jnp.bfloat16)

    def near_only(h):
        key = turned(k_ref[:, head_at(h)], my_rows).astype(jnp.bfloat16)
        maps = []
        for query in queries_of(h):
            scores = jnp.where(visible, product(query, key), neg_large)
            powers = jnp.exp(scores - jnp.max(scores, axis=-1, keepdims=True))
            maps.append((powers, jnp.sum(powers, axis=-1, keepdims=True)))
        (first, first_sum), (second, second_sum) = maps
        weights = first * (1.0 / first_sum) - second * (mix_ref[h] / second_sum)
        finish(
            h,
            jnp.dot(weights.astype(jnp.bfloat16), v_ref[:, head_at(h)], preferred_element_type=jnp.float32),
        )

    def near_and_far(h):
        key = turned(k_ref[:, head_at(h)], my_rows).astype(jnp.bfloat16)
        far_key = turned(far_k[:, head_at(h)], pl.ds(0, tokens)).astype(jnp.bfloat16)
        maps = []
        for query in queries_of(h):
            scores = jnp.where(visible, product(query, key), neg_large)
            far_scores = product(query, far_key)
            highest = jnp.maximum(
                jnp.max(scores, axis=-1, keepdims=True), jnp.max(far_scores, axis=-1, keepdims=True)
            )
            powers = jnp.exp(scores - highest)
            far_powers = jnp.exp(far_scores - highest)
            total = jnp.sum(powers, axis=-1, keepdims=True) + jnp.sum(far_powers, axis=-1, keepdims=True)
            maps.append((powers, far_powers, total))
        (first, far_first, first_sum), (second, far_second, second_sum) = maps
        one, two = 1.0 / first_sum, mix_ref[h] / second_sum
        weights = (first * one - second * two).astype(jnp.bfloat16)
        far_weights = (far_first * one - far_second * two).astype(jnp.bfloat16)
        finish(
            h,
            jnp.dot(weights, v_ref[:, head_at(h)], preferred_element_type=jnp.float32)
            + jnp.dot(far_weights, far_v[:, head_at(h)], preferred_element_type=jnp.float32),
        )

    def head_step(h, carry):
        for when, action in events:
            turn = max(0, int(when))
            if turn < heads:
                pl.when(h == turn)(action)

        @pl.when(s == 0)
        def _():
            near_only(h)

        @pl.when(s == 1)
        def _():
            far_copy(h, k_ref, far_k, k_send, k_recv).wait_recv()
            far_copy(h, v_ref, far_v, v_send, v_recv).wait_recv()
            near_and_far(h)

        return carry

    lax.fori_loop(0, heads, head_step, 0)
    own_copy.wait()

    def project(zz, yy):
        for q in range(pieces):
            arrived(zz, yy, 1 - c, q)
        chip = pl.ds(pl.multiple_of((zz * 2 + yy) * 2 * columns, 2 * columns), 2 * columns)
        out_ref[:, chip] = jnp.dot(
            attended[...], wall[:, chip], preferred_element_type=jnp.float32
        ).astype(out_ref.dtype)

    orders = [sorted(range(depth_z), key=lambda b: (abs(b - a), b)) for a in range(depth_z)]
    sides = []
    for a, order in enumerate(orders):
        b = a + 1 - 2 * (a % 2)
        sides.append([o for o in order[:-1] if o != b] + [b, order[-1]])
    last = block_time * depth_z + 2.0
    for n in range(depth_z):
        zz = pick([order[n] for order in orders], z)
        side = pick([order[n] for order in sides], z)
        early = heads + 0.01 * n
        line_time = max(early, block_time * n + 0.05)
        side_time = max(early + 0.005, block_time * (n + 2 if n else 1) + 1.05)
        if n >= depth_z - 2:
            side_time = last + 0.01 * n
        events.append((line_time, functools.partial(project, zz, y)))
        events.append((side_time, functools.partial(project, side, 1 - y)))
    events.sort(key=lambda e: e[0])
    for when, action in events:
        if max(0, int(when)) >= heads:
            action()

    for q in range(pieces):
        for b in range(depth_z):
            passed_up = (b <= z) & (z < depth_z - 1)
            passed_down = (b >= z) & (z > 0)

            @pl.when(passed_up)
            def _(b=b):
                to_up(b, q).wait_send()

            @pl.when(passed_down)
            def _(b=b):
                to_down(b, q).wait_send()

            if q < late:
                to_side(b, q).wait_send()
            else:

                @pl.when(b != near)
                def _(b=b):
                    to_side(b, q).wait_send()

            for yy in range(2):
                to_core(b, yy, q).wait_send()
        if q >= late:
            to_near(q).wait_send()

    @pl.when(s == 0)
    def _():
        def ended(h, carry):
            far_copy(h, k_ref, far_k, k_send, k_recv).wait_send()
            far_copy(h, v_ref, far_v, v_send, v_recv).wait_send()
            return carry

        lax.fori_loop(0, heads, ended, 0)


def lines_of(mesh):
    names = tuple(mesh.axis_names)
    if names != ("sp", "dp") or mesh.shape["sp"] != 2 or mesh.shape["dp"] % 4:
        return None
    depth_z = mesh.shape["dp"] // 4
    return depth_z if depth_z >= 4 and depth_z % 2 == 0 else None


def on_line(depth_z, queries, keys, values, mix_ratio, out_gain, out_weight):
    _, tokens, heads, size = queries.shape
    features = heads * size
    pieces = 4
    cosine, sine = rotation_tables(2 * tokens, size // 2)
    raw = [field.reshape(tokens, heads, size) for field in (queries, keys, values)]
    vmem = pl.BlockSpec(memory_space=pltpu.VMEM)
    smem = pl.BlockSpec(memory_space=pltpu.SMEM)
    far = pl.BlockSpec(memory_space=pl.ANY)
    dma = pltpu.SemaphoreType.DMA
    result = pl.pallas_call(
        functools.partial(line_kernel, depth_z, heads, pieces),
        out_shape=jax.ShapeDtypeStruct((tokens, features), jnp.bfloat16),
        in_specs=[smem, far, far, far, far, far, vmem, vmem, far],
        out_specs=vmem,
        scratch_shapes=[
            pltpu.VMEM((tokens, heads, size), jnp.bfloat16),
            pltpu.VMEM((tokens, heads, size), jnp.bfloat16),
            pltpu.VMEM((tokens, heads, size), jnp.bfloat16),
            pltpu.VMEM(cosine.shape, jnp.float32),
            pltpu.VMEM(sine.shape, jnp.float32),
            pltpu.VMEM(out_weight.shape, jnp.bfloat16),
            pltpu.VMEM((tokens, features), jnp.bfloat16),
            pltpu.VMEM((tokens, features), jnp.bfloat16),
            pltpu.VMEM((tokens, features), jnp.bfloat16),
            pltpu.VMEM((tokens, features), jnp.bfloat16),
            pltpu.VMEM((tokens, features), jnp.bfloat16),
            pltpu.VMEM((features, out_weight.shape[1] * depth_z * 4), jnp.bfloat16),
            pltpu.VMEM((tokens, features), jnp.bfloat16),
            dma((6,)),
            dma((heads,)),
            dma((heads,)),
            dma((heads,)),
            dma((heads,)),
            dma((depth_z, 2, 2, pieces)),
            dma((depth_z, pieces)),
            dma((depth_z, pieces)),
            dma((depth_z, pieces)),
            dma((depth_z, 2, pieces)),
            dma((pieces,)),
            dma,
        ],
        compiler_params=pltpu.CompilerParams(
            collective_id=0, has_side_effects=True, vmem_limit_bytes=56 * 2**20
        ),
    )(
        mix_ratio,
        *raw,
        jnp.asarray(cosine),
        jnp.asarray(sine),
        jnp.asarray(turning_matrix(size // 2), jnp.bfloat16),
        out_gain.reshape(1, size),
        out_weight,
    )
    return result.reshape(1, tokens, features)


def solution(mesh):
    in_specs = (
        P("dp", "sp", None, None),
        P("dp", "sp", None, None),
        P("dp", "sp", None, None),
        P(),
        P(),
        P(None, "dp"),
    )
    out_specs = P("dp", "sp", None)
    depth_z = lines_of(mesh)

    def body(queries, *rest):
        fits = depth_z is not None and queries.shape[0] == 1 and queries.shape[1] <= 256
        return functools.partial(on_line, depth_z)(queries, *rest) if fits else on_device(queries, *rest)

    return jax.shard_map(body, mesh=mesh, in_specs=in_specs, out_specs=out_specs, check_vma=False)
```

```python
import functools
import math

import jax
import jax.numpy as jnp
import numpy as np
from jax import lax
from jax.experimental import pallas as pl
from jax.experimental.pallas import tpu as pltpu
from jax.sharding import PartitionSpec as P

theta_base = 500000.0
neg_large = -1e30
norm_eps = 1e-05
MESH = pl.DeviceIdType.MESH


def rotate_halves(field, positions):
    width = field.shape[-1] // 2
    half = width // 2
    freqs = theta_base ** (-jnp.arange(half, dtype=jnp.float32) * 2.0 / width)
    angle = positions.astype(jnp.float32)[:, None] * freqs[None, :]
    cosine = jnp.cos(angle)[:, None, :]
    sine = jnp.sin(angle)[:, None, :]
    parts = field.reshape(field.shape[0], 2, width)
    lower = parts[..., :half]
    upper = parts[..., half:]
    turned = jnp.concatenate(
        [lower * cosine - upper * sine, upper * cosine + lower * sine], axis=-1
    )
    return turned.reshape(field.shape)


def masked_softmax(scores, visible):
    kept = jnp.where(visible, scores, neg_large)
    highest = jnp.max(kept, axis=-1, keepdims=True)
    powers = jnp.exp(kept - highest)
    return powers / jnp.sum(powers, axis=-1, keepdims=True)


def head_attention(query_head, key_head, value_head, ratio, gain):
    length = query_head.shape[0]
    width = query_head.shape[1] // 2
    positions = jnp.arange(length, dtype=jnp.int32)
    rotated_queries = (
        rotate_halves(query_head.astype(jnp.float32), positions) * width ** (-0.5)
    ).astype(jnp.bfloat16)
    rotated_keys = rotate_halves(key_head.astype(jnp.float32), positions).astype(jnp.bfloat16)
    block = math.gcd(512, length)

    def one_block(start):
        query_rows = lax.dynamic_slice_in_dim(rotated_queries, start, block, 0)
        visible = (start + jnp.arange(block, dtype=jnp.int32))[:, None] >= positions[None, :]
        first = jnp.dot(
            query_rows[:, :width], rotated_keys[:, :width].T, preferred_element_type=jnp.float32
        )
        second = jnp.dot(
            query_rows[:, width:], rotated_keys[:, width:].T, preferred_element_type=jnp.float32
        )
        weights = (masked_softmax(first, visible) - ratio * masked_softmax(second, visible)).astype(
            jnp.bfloat16
        )
        mixed = jnp.dot(weights, value_head, preferred_element_type=jnp.float32)
        scale = lax.rsqrt(jnp.mean(mixed * mixed, axis=-1, keepdims=True) + norm_eps)
        return (mixed * scale * gain).astype(jnp.bfloat16)

    starts = jnp.arange(length // block, dtype=jnp.int32) * block
    return lax.map(one_block, starts).reshape(length, value_head.shape[1])


def on_device(queries, keys, values, mix_ratio, out_gain, out_weight):
    groups = lax.axis_size("sp")
    heads_here = queries.shape[2] // groups
    query_all, key_all, value_all = (
        lax.all_to_all(queries, "sp", split_axis=2, concat_axis=1, tiled=True),
        lax.all_to_all(keys, "sp", split_axis=2, concat_axis=1, tiled=True),
        lax.all_to_all(values, "sp", split_axis=2, concat_axis=1, tiled=True),
    )
    seqs = query_all.shape[0]
    length = query_all.shape[1]
    first_head = lax.axis_index("sp") * heads_here
    ratios = lax.dynamic_slice_in_dim(mix_ratio, first_head, heads_here, 0)
    item_ratios = jnp.tile(ratios, seqs)

    def by_item(field):
        return jnp.swapaxes(field, 1, 2).reshape(seqs * heads_here, length, field.shape[3])

    def one_head(head_items):
        query_head, key_head, value_head, ratio = head_items
        return head_attention(query_head, key_head, value_head, ratio, out_gain)

    heads = lax.map(
        one_head, (by_item(query_all), by_item(key_all), by_item(value_all), item_ratios)
    )
    attended = jnp.swapaxes(heads.reshape(seqs, heads_here, length, heads.shape[2]), 1, 2)
    returned = lax.all_to_all(attended, "sp", split_axis=1, concat_axis=2, tiled=True)
    tokens_here = returned.shape[1]
    token_rows = returned.reshape(seqs * tokens_here, -1)
    result = jnp.dot(
        token_rows,
        lax.all_gather(out_weight, "dp", axis=1, tiled=True),
        preferred_element_type=jnp.float32,
    ).astype(jnp.bfloat16)
    return result.reshape(seqs, tokens_here, -1)


def rotation_tables(length, width):
    half = width // 2
    freqs = theta_base ** (-np.arange(half, dtype=np.float32) * np.float32(2.0) / width)
    angle = np.arange(length, dtype=np.float32)[:, None] * freqs.astype(np.float32)[None, :]
    cosine, sine = np.cos(angle), np.sin(angle)
    return (
        np.tile(cosine, (1, 4)).astype(np.float32),
        np.tile(sine, (1, 4)).astype(np.float32),
    )


def turning_matrix(width):
    half = width // 2
    turn = np.zeros((2 * width, 2 * width), np.float32)
    for part in range(2):
        for j in range(half):
            turn[part * width + half + j, part * width + j] = -1.0
            turn[part * width + j, part * width + half + j] = 1.0
    return turn


def pick(table, index):
    value = jnp.int32(table[0])
    for i, entry in enumerate(table[1:], 1):
        value = jnp.where(index == i, jnp.int32(entry), value)
    return value


def line_kernel(
    depth_z, heads, pieces, mix_ref, q_in, k_in, v_in, cos_in, sin_in, turn_ref, gain_ref, w_in,
    out_ref, q_raw, k_raw, v_raw, cos_ref, sin_ref, w_ref, q_ref, k_ref, v_ref, far_k, far_v, wall, attended, in_sems,
    k_send, v_send, k_recv, v_recv, w_recv, up_send, down_send, side_send, core_send, extra_send, own_sem,
):
    s = lax.axis_index("sp")
    d = lax.axis_index("dp")
    c = lax.rem(d, 2)
    y = lax.rem(d // 2, 2)
    z = d // 4
    tokens = q_ref.shape[0]
    size = q_ref.shape[1] // heads
    width = size // 2
    columns = w_ref.shape[1]
    rows = w_ref.shape[0] // pieces

    def at(zz, yy, cc):
        return {"sp": s, "dp": (zz * 2 + yy) * 2 + cc}

    across = {"sp": 1 - s, "dp": d}
    loads = [
        pltpu.make_async_copy(src, dst, in_sems.at[i])
        for i, (src, dst) in enumerate(
            [(w_in, w_ref), (k_in, k_raw), (v_in, v_raw), (q_in, q_raw), (cos_in, cos_ref), (sin_in, sin_ref)]
        )
    ]
    for load in loads:
        load.start()
    barrier = pltpu.get_barrier_semaphore()

    def greet(target):
        pl.semaphore_signal(barrier, inc=1, device_id=target, device_id_type=MESH)

    greet(across)
    greet(at(z, 1 - y, c))
    greet(at(z, y, 1 - c))

    @pl.when(z > 0)
    def _():
        greet(at(z - 1, y, c))

    @pl.when(z < depth_z - 1)
    def _():
        greet(at(z + 1, y, c))

    pl.semaphore_wait(
        barrier,
        3 + jnp.where(z > 0, 1, 0).astype(jnp.int32) + jnp.where(z < depth_z - 1, 1, 0).astype(jnp.int32),
    )

    loads[0].wait()

    def place(zz, yy, cc, q):
        column = pl.multiple_of(((zz * 2 + yy) * 2 + cc) * columns, columns)
        return wall.at[pl.ds(q * rows, rows), pl.ds(column, columns)]

    def send(zz, yy, cc, q, sem, target, own):
        where = place(zz, yy, cc, q)
        return pltpu.make_async_remote_copy(
            src_ref=w_ref.at[pl.ds(q * rows, rows), :] if own else where,
            dst_ref=where,
            send_sem=sem,
            recv_sem=w_recv.at[zz, yy, cc, q],
            device_id=target,
            device_id_type=MESH,
        )

    near = z + 1 - 2 * lax.rem(z, 2)

    def to_up(zz, q, own=False):
        return send(zz, y, c, q, up_send.at[zz, q], at(z + 1, y, c), own)

    def to_down(zz, q, own=False):
        return send(zz, y, c, q, down_send.at[zz, q], at(z - 1, y, c), own)

    def to_side(zz, q, own=False):
        return send(zz, y, c, q, side_send.at[zz, q], at(z, 1 - y, c), own)

    def to_core(zz, yy, q, own=False):
        return send(zz, yy, c, q, core_send.at[zz, yy, q], at(z, y, 1 - c), own)

    def to_near(q):
        return send(z, 1 - y, c, q, extra_send.at[q], at(near, y, c), False)

    def arrived(zz, yy, cc, q):
        send(zz, yy, cc, q, side_send.at[0, 0], at(z, 1 - y, c), False).wait_recv()

    def head_at(h):
        return pl.ds(pl.multiple_of(h * size, size), size)

    def far_copy(h, src, dst, sends, recvs):
        return pltpu.make_async_remote_copy(
            src_ref=src.at[:, head_at(h)],
            dst_ref=dst.at[:, head_at(h)],
            send_sem=sends.at[h],
            recv_sem=recvs.at[h],
            device_id=across,
            device_id_type=MESH,
        )

    for q in range(pieces):

        @pl.when(z > 0)
        def _(q=q):
            to_down(z, q, True).start()

        @pl.when(z < depth_z - 1)
        def _(q=q):
            to_up(z, q, True).start()

        to_side(z, q, True).start()
        to_core(z, y, q, True).start()

    def flatten(src, dst):
        rows_now = math.gcd(16, tokens)

        def some(i, carry):
            part = pl.ds(pl.multiple_of(i * rows_now, rows_now), rows_now)
            dst[part, :] = src[part, :, :].reshape(rows_now, heads * size)
            return carry

        lax.fori_loop(0, tokens // rows_now, some, 0)

    for load, src, dst in ((loads[1], k_raw, k_ref), (loads[2], v_raw, v_ref), (loads[3], q_raw, q_ref)):
        load.wait()
        flatten(src, dst)

    @pl.when(s == 0)
    def _():
        def start(h, carry):
            far_copy(h, k_ref, far_k, k_send, k_recv).start()
            far_copy(h, v_ref, far_v, v_send, v_recv).start()
            return carry

        lax.fori_loop(0, heads, start, 0)

    own_copy = pltpu.make_async_copy(
        w_ref, wall.at[:, pl.ds(pl.multiple_of(d * columns, columns), columns)], own_sem
    )
    own_copy.start()
    loads[4].wait()
    loads[5].wait()

    late = pieces // 2

    def line_arrival(r, q):
        for sign in (-1, 1):
            zz = z + sign * r

            @pl.when((zz >= 0) & (zz < depth_z))
            def _(zz=zz, sign=sign):
                arrived(zz, y, c, q)
                if sign < 0:

                    @pl.when(z < depth_z - 1)
                    def _():
                        to_up(zz, q).start()
                else:

                    @pl.when(z > 0)
                    def _():
                        to_down(zz, q).start()

                if q < late:
                    to_side(zz, q).start()
                else:

                    @pl.when(zz != near)
                    def _():
                        to_side(zz, q).start()

                to_core(zz, y, q).start()

    def side_arrival(r, q):
        if r == 0:
            arrived(z, 1 - y, c, q)
            to_core(z, 1 - y, q).start()
            return
        for sign in (-1, 1):
            zz = z + sign * r
            here = (zz >= 0) & (zz < depth_z)
            if q >= late:
                here = here & (zz != near)

            @pl.when(here)
            def _(zz=zz):
                arrived(zz, 1 - y, c, q)
                to_core(zz, 1 - y, q).start()

    def extra(q):
        to_near(q).start()

    def extra_arrival(q):
        arrived(near, 1 - y, c, q)
        to_core(near, 1 - y, q).start()

    block_time = 4.0 * heads / 12.0
    events = []
    for q in range(pieces):
        step = (q + 1) / pieces
        for r in range(1, depth_z):
            events.append((block_time * (r - 1 + step), functools.partial(line_arrival, r, q)))
            events.append((block_time * (r + step) + 1.0, functools.partial(side_arrival, r, q)))
        events.append((block_time * step + 1.0, functools.partial(side_arrival, 0, q)))
        if q >= late:
            events.append((block_time * (depth_z - 2) + 0.5 + 0.01 * q, functools.partial(extra, q)))
            events.append((block_time * (depth_z - 1 + step) + 1.5, functools.partial(extra_arrival, q)))
    events.sort(key=lambda e: e[0])

    lane = lax.broadcasted_iota(jnp.int32, (tokens, size), 1)
    visible = lax.broadcasted_iota(jnp.int32, (tokens, tokens), 0) >= lax.broadcasted_iota(
        jnp.int32, (tokens, tokens), 1
    )
    my_rows = pl.ds(pl.multiple_of(s * tokens, 8), tokens)

    def turned(field, table_rows):
        crossed = jnp.dot(field, turn_ref[...], preferred_element_type=jnp.float32)
        return field.astype(jnp.float32) * cos_ref[table_rows, :] + crossed * sin_ref[table_rows, :]

    def product(a, b):
        return lax.dot_general(a, b, (((1,), (1,)), ((), ())), preferred_element_type=jnp.float32)

    def queries_of(h):
        query = (turned(q_ref[:, head_at(h)], my_rows) * width ** (-0.5)).astype(jnp.bfloat16)
        zero = jnp.zeros_like(query)
        return jnp.where(lane < width, query, zero), jnp.where(lane < width, zero, query)

    def finish(h, mixed):
        scale = lax.rsqrt(jnp.mean(mixed * mixed, axis=-1, keepdims=True) + norm_eps)
        attended[:, head_at(h)] = (mixed * scale * gain_ref[...]).astype(jnp.bfloat16)

    def near_only(h):
        key = turned(k_ref[:, head_at(h)], my_rows).astype(jnp.bfloat16)
        maps = []
        for query in queries_of(h):
            scores = jnp.where(visible, product(query, key), neg_large)
            powers = jnp.exp(scores - jnp.max(scores, axis=-1, keepdims=True))
            maps.append((powers, jnp.sum(powers, axis=-1, keepdims=True)))
        (first, first_sum), (second, second_sum) = maps
        weights = first * (1.0 / first_sum) - second * (mix_ref[h] / second_sum)
        finish(
            h,
            jnp.dot(weights.astype(jnp.bfloat16), v_ref[:, head_at(h)], preferred_element_type=jnp.float32),
        )

    def near_and_far(h):
        key = turned(k_ref[:, head_at(h)], my_rows).astype(jnp.bfloat16)
        far_key = turned(far_k[:, head_at(h)], pl.ds(0, tokens)).astype(jnp.bfloat16)
        maps = []
        for query in queries_of(h):
            scores = jnp.where(visible, product(query, key), neg_large)
            far_scores = product(query, far_key)
            highest = jnp.maximum(
                jnp.max(scores, axis=-1, keepdims=True), jnp.max(far_scores, axis=-1, keepdims=True)
            )
            powers = jnp.exp(scores - highest)
            far_powers = jnp.exp(far_scores - highest)
            total = jnp.sum(powers, axis=-1, keepdims=True) + jnp.sum(far_powers, axis=-1, keepdims=True)
            maps.append((powers, far_powers, total))
        (first, far_first, first_sum), (second, far_second, second_sum) = maps
        one, two = 1.0 / first_sum, mix_ref[h] / second_sum
        weights = (first * one - second * two).astype(jnp.bfloat16)
        far_weights = (far_first * one - far_second * two).astype(jnp.bfloat16)
        finish(
            h,
            jnp.dot(weights, v_ref[:, head_at(h)], preferred_element_type=jnp.float32)
            + jnp.dot(far_weights, far_v[:, head_at(h)], preferred_element_type=jnp.float32),
        )

    def head_step(h, carry):
        for when, action in events:
            turn = max(0, int(when))
            if turn < heads:
                pl.when(h == turn)(action)

        @pl.when(s == 0)
        def _():
            near_only(h)

        @pl.when(s == 1)
        def _():
            far_copy(h, k_ref, far_k, k_send, k_recv).wait_recv()
            far_copy(h, v_ref, far_v, v_send, v_recv).wait_recv()
            near_and_far(h)

        return carry

    lax.fori_loop(0, heads, head_step, 0)
    own_copy.wait()

    def project(zz, yy):
        for q in range(pieces):
            arrived(zz, yy, 1 - c, q)
        chip = pl.ds(pl.multiple_of((zz * 2 + yy) * 2 * columns, 2 * columns), 2 * columns)
        out_ref[:, chip] = jnp.dot(
            attended[...], wall[:, chip], preferred_element_type=jnp.float32
        ).astype(out_ref.dtype)

    orders = [sorted(range(depth_z), key=lambda b: (abs(b - a), b)) for a in range(depth_z)]
    sides = []
    for a, order in enumerate(orders):
        b = a + 1 - 2 * (a % 2)
        sides.append([o for o in order[:-1] if o != b] + [b, order[-1]])
    last = block_time * depth_z + 2.0
    for n in range(depth_z):
        zz = pick([order[n] for order in orders], z)
        side = pick([order[n] for order in sides], z)
        early = heads + 0.01 * n
        line_time = max(early, block_time * n + 0.05)
        side_time = max(early + 0.005, block_time * (n + 2 if n else 1) + 1.05)
        if n >= depth_z - 2:
            side_time = last + 0.01 * n
        events.append((line_time, functools.partial(project, zz, y)))
        events.append((side_time, functools.partial(project, side, 1 - y)))
    events.sort(key=lambda e: e[0])
    for when, action in events:
        if max(0, int(when)) >= heads:
            action()

    for q in range(pieces):
        for b in range(depth_z):
            passed_up = (b <= z) & (z < depth_z - 1)
            passed_down = (b >= z) & (z > 0)

            @pl.when(passed_up)
            def _(b=b):
                to_up(b, q).wait_send()

            @pl.when(passed_down)
            def _(b=b):
                to_down(b, q).wait_send()

            if q < late:
                to_side(b, q).wait_send()
            else:

                @pl.when(b != near)
                def _(b=b):
                    to_side(b, q).wait_send()

            for yy in range(2):
                to_core(b, yy, q).wait_send()
        if q >= late:
            to_near(q).wait_send()

    @pl.when(s == 0)
    def _():
        def ended(h, carry):
            far_copy(h, k_ref, far_k, k_send, k_recv).wait_send()
            far_copy(h, v_ref, far_v, v_send, v_recv).wait_send()
            return carry

        lax.fori_loop(0, heads, ended, 0)


def lines_of(mesh):
    names = tuple(mesh.axis_names)
    if names != ("sp", "dp") or mesh.shape["sp"] != 2 or mesh.shape["dp"] % 4:
        return None
    depth_z = mesh.shape["dp"] // 4
    return depth_z if depth_z >= 4 and depth_z % 2 == 0 else None


def on_line(depth_z, queries, keys, values, mix_ratio, out_gain, out_weight):
    _, tokens, heads, size = queries.shape
    features = heads * size
    pieces = 4
    cosine, sine = rotation_tables(2 * tokens, size // 2)
    raw = [field.reshape(tokens, heads, size) for field in (queries, keys, values)]
    vmem = pl.BlockSpec(memory_space=pltpu.VMEM)
    smem = pl.BlockSpec(memory_space=pltpu.SMEM)
    far = pl.BlockSpec(memory_space=pl.ANY)
    dma = pltpu.SemaphoreType.DMA
    result = pl.pallas_call(
        functools.partial(line_kernel, depth_z, heads, pieces),
        out_shape=pltpu.VMEM((tokens, features), jnp.bfloat16),
        in_specs=[smem, far, far, far, far, far, vmem, vmem, far],
        out_specs=vmem,
        scratch_shapes=[
            pltpu.VMEM((tokens, heads, size), jnp.bfloat16),
            pltpu.VMEM((tokens, heads, size), jnp.bfloat16),
            pltpu.VMEM((tokens, heads, size), jnp.bfloat16),
            pltpu.VMEM(cosine.shape, jnp.float32),
            pltpu.VMEM(sine.shape, jnp.float32),
            pltpu.VMEM(out_weight.shape, jnp.bfloat16),
            pltpu.VMEM((tokens, features), jnp.bfloat16),
            pltpu.VMEM((tokens, features), jnp.bfloat16),
            pltpu.VMEM((tokens, features), jnp.bfloat16),
            pltpu.VMEM((tokens, features), jnp.bfloat16),
            pltpu.VMEM((tokens, features), jnp.bfloat16),
            pltpu.VMEM((features, out_weight.shape[1] * depth_z * 4), jnp.bfloat16),
            pltpu.VMEM((tokens, features), jnp.bfloat16),
            dma((6,)),
            dma((heads,)),
            dma((heads,)),
            dma((heads,)),
            dma((heads,)),
            dma((depth_z, 2, 2, pieces)),
            dma((depth_z, pieces)),
            dma((depth_z, pieces)),
            dma((depth_z, pieces)),
            dma((depth_z, 2, pieces)),
            dma((pieces,)),
            dma,
        ],
        compiler_params=pltpu.CompilerParams(
            collective_id=0, has_side_effects=True, vmem_limit_bytes=56 * 2**20
        ),
    )(
        mix_ratio,
        *raw,
        jnp.asarray(cosine),
        jnp.asarray(sine),
        jnp.asarray(turning_matrix(size // 2), jnp.bfloat16),
        out_gain.reshape(1, size),
        out_weight,
    )
    return result.reshape(1, tokens, features)


def solution(mesh):
    in_specs = (
        P("dp", "sp", None, None),
        P("dp", "sp", None, None),
        P("dp", "sp", None, None),
        P(),
        P(),
        P(None, "dp"),
    )
    out_specs = P("dp", "sp", None)
    depth_z = lines_of(mesh)

    def body(queries, *rest):
        fits = depth_z is not None and queries.shape[0] == 1 and queries.shape[1] <= 256
        return functools.partial(on_line, depth_z)(queries, *rest) if fits else on_device(queries, *rest)

    return jax.shard_map(body, mesh=mesh, in_specs=in_specs, out_specs=out_specs, check_vma=False)
```
